32 devices in a mesh: grp: 2 (over x), fs: 4 (over y, core), tp: 4 (over z).
Axes of the slice: x: 2, y: 2, z: 4, core: 2. Of those that a mesh axis runs over, the one named last changes fastest.
Arguments:
- prompt_tokens: bfloat16 [4096, 2048], P(('grp', 'fs', 'tp')), parts along dimension 0, may hold values from -6 to 6
- up_weight: float32 [2048, 8192], P('fs', 'tp'), may hold values from -0.125 to 0.125
- down_weight: float32 [2048, 8192], P('fs', 'tp'), may hold values from -0.0625 to 0.0625
- pre_gain: float32 [2048], P('fs'), may hold values from 0.1 to 1.9
- post_gain: float32 [2048], replicated, may hold values from 0.1 to 1.9
Outputs:
- mixed: bfloat16 [4096, 2048], P(('grp', 'fs', 'tp')), parts along dimension 0
- sampler_up: bfloat16 [4096, 8192], P('grp', 'tp'), parts along dimension 0
- sampler_down: bfloat16 [4096, 8192], P('grp', 'tp'), parts along dimension 0
The draws below stay inside these ranges and needn't reach their ends.
There are 2 independent parts, one for each index of `grp`. The reference program is written for one: setup_inputs(seed, part) draws one part's arguments, and reference() takes and returns one part's arrays. A program takes and returns all parts, laid end to end along the dimension named above; an argument that names none is the same for every part. Nothing has to cross between parts.
All inputs are finite; a program needn't handle non-finite values.
Results may differ from the reference program's by a relative error of at most 0.015.
Values may be sent and summed in bfloat16 or wider, within the bound.
No kernel may reach another device: no remote copies, remote signals or barrier semaphores. Data moves between devices by JAX's collectives and lax.ppermute only.
A program may use at most 128 MiB of HBM per device.

```python
import jax
import jax.numpy as jnp
from jax import lax

D = 2048
FF = 8192
TOK_DEV = 128
TOKENS = 2048
N_TP = 4


def shard_levels(stream_key, extent, split, low, top_value):
    loudness = 1.0
    for dim, blocks in split:
        heights = jax.random.uniform(jax.random.fold_in(jax.random.fold_in(stream_key, 6), dim), (blocks,), jnp.float32, low / len(split), top_value / len(split))
        loudness = loudness * jnp.repeat(jnp.exp(heights), extent[dim] // blocks).reshape((-1,) + (1,) * (len(extent) - 1 - dim))
    return loudness


def gaussian(key, shape, scale, reach, shards=(), dtype=jnp.bfloat16):
    values = jax.random.normal(key, shape, jnp.float32) * scale
    if len(shards) > 0:
        values = shard_levels(key, shape, shards, -0.22, 0.18) * values
    return jnp.clip(values, min=-reach, max=reach).astype(dtype)


def setup_inputs(seed: int = 0, part: int = 0) -> dict:
    arg_keys = jax.random.split(jax.random.key(seed), 6)
    part_splits = jax.random.split(jax.random.fold_in(arg_keys[5], part), 6)
    return {
        "prompt_tokens": gaussian(part_splits[0], (TOKENS, D), 1.0, 6.0, ((0, 16),)),
        "up_weight": gaussian(arg_keys[1], (D, FF), D ** -0.5, 0.125, ((0, 4), (1, 4)), jnp.float32),
        "down_weight": gaussian(arg_keys[2], (D, FF), FF ** -0.5, 0.0625, ((0, 4), (1, 4)), jnp.float32),
        "pre_gain": jnp.clip(1.0 + 0.18 * jax.random.normal(arg_keys[3], (D,), jnp.float32), 0.1, 1.9),
        "post_gain": jnp.clip(1.0 + 0.18 * jax.random.normal(arg_keys[4], (D,), jnp.float32), 0.1, 1.9),
    }


def reference(prompt_tokens, up_weight, down_weight, pre_gain, post_gain):
    sampler_up = (up_weight * pre_gain[:, None]).astype(jnp.bfloat16)
    sampler_down = down_weight.astype(jnp.bfloat16)
    width = prompt_tokens.shape[1]
    hidden_units = up_weight.shape[1]
    block_rows = TOK_DEV * N_TP
    blocks = prompt_tokens.reshape(TOKENS // block_rows, block_rows, width)
    down_split = sampler_down.astype(jnp.float32).reshape(width, N_TP, hidden_units // N_TP)

    def one_block(rows):
        values = rows.astype(jnp.float32)
        normed = (values * lax.rsqrt(lax.optimization_barrier(jnp.mean(values * values, axis=1, keepdims=True)) + 1e-06)).astype(jnp.bfloat16)
        lifted = jnp.dot(normed, sampler_up, preferred_element_type=jnp.float32)
        hidden = jnp.square(jax.nn.relu(lifted)).astype(jnp.bfloat16)
        hidden_split = hidden.astype(jnp.float32).reshape(block_rows, N_TP, hidden_units // N_TP)
        parts = jnp.einsum('rbk,dbk->brd', hidden_split, down_split).astype(jnp.bfloat16)
        summed = lax.optimization_barrier(jnp.sum(parts.astype(jnp.float32), axis=0))
        scaled = summed * lax.rsqrt(lax.optimization_barrier(jnp.mean(summed * summed, axis=1, keepdims=True)) + 1e-06)
        return (scaled * post_gain[None, :]).astype(jnp.bfloat16)
    mixed = lax.map(one_block, blocks).reshape(TOKENS, width)
    return (mixed, sampler_up, sampler_down)
```

```python
import jax
import jax.numpy as jnp
from jax import lax
from jax.experimental import pallas as pl
from jax.experimental.pallas import tpu as pltpu
from jax.sharding import PartitionSpec as P


BF = jnp.bfloat16
F32 = jnp.float32
ANY = pl.BlockSpec(memory_space=pl.ANY)
SMEM = pl.BlockSpec(memory_space=pltpu.SMEM)
LIMIT = pltpu.CompilerParams(vmem_limit_bytes=48 * 2**20)


def plain(prompt_tokens, up_weight, down_weight, pre_gain, post_gain):
    up_local = (up_weight * pre_gain[:, None]).astype(BF)
    down_local = down_weight.astype(BF)
    values = prompt_tokens.astype(F32)
    normed = (
        values * lax.rsqrt(jnp.mean(values * values, axis=1, keepdims=True) + 1e-06)
    ).astype(BF)
    sampler_up = lax.all_gather(up_local, "fs", axis=0, tiled=True)
    sampler_down = lax.all_gather(down_local, "fs", axis=0, tiled=True)
    lifted = jnp.dot(
        lax.all_gather(normed, "tp", axis=0, tiled=True),
        sampler_up,
        preferred_element_type=F32,
    )
    hidden = jnp.square(jax.nn.relu(lifted)).astype(BF)
    part = lax.dot_general(
        hidden, sampler_down, (((1,), (1,)), ((), ())), preferred_element_type=F32
    )
    summed = lax.psum_scatter(
        part.astype(BF), "tp", scatter_dimension=0, tiled=True
    ).astype(F32)
    scaled = summed * lax.rsqrt(jnp.mean(summed * summed, axis=1, keepdims=True) + 1e-06)
    return (scaled * post_gain[None, :]).astype(BF), sampler_up, sampler_down


def norm_tokens(tokens, starts, sizes):
    n, width = tokens.shape

    def body(at, x, o, buf):
        v = x[...].astype(F32)
        buf[...] = (v * lax.rsqrt(jnp.mean(v * v, axis=1, keepdims=True) + 1e-06)).astype(BF)
        col = 0
        for p, size in enumerate(sizes):
            o[:, col : col + size] = buf[:, pl.ds(pl.multiple_of(at[p], 128), size)]
            col += size

    return pl.pallas_call(
        body,
        out_shape=jax.ShapeDtypeStruct((n, width), BF),
        in_specs=[SMEM, pl.BlockSpec(memory_space=pltpu.VMEM)],
        out_specs=pl.BlockSpec(memory_space=pltpu.VMEM),
        scratch_shapes=[pltpu.VMEM((n, width), BF)],
        name="norm_tokens",
    )(starts, tokens)


def up_tile(blocks, pieces, starts, j, n_tiles, hidden, whole, rows, sub=256):
    tok, width = blocks[0].shape
    n_tok = tok * len(blocks)
    hid = pieces[0].shape[1]
    tile = hid // n_tiles
    steps = tile // sub
    n, nb = len(pieces), len(blocks)
    sizes = [p.shape[0] for p in pieces]

    def body(*refs):
        at, toks, ins = refs[0], refs[1 : 1 + nb], refs[1 + nb : 1 + nb + n]
        o, whole_out, x, sem = refs[-4:]
        i = pl.program_id(0)

        @pl.when(i == 0)
        def _():
            for b in range(nb):
                x[b * tok : (b + 1) * tok, :] = toks[b][...]

        copies = []
        for p in range(n):
            c = pltpu.make_async_copy(
                ins[p],
                whole_out.at[
                    pl.ds(pl.multiple_of(at[p], 16), sizes[p]),
                    pl.ds(pl.multiple_of(j * tile + i * sub, sub), sub),
                ],
                sem.at[p],
            )
            c.start()
            copies.append(c)
        total, c0 = None, 0
        for p in range(n):
            term = jnp.dot(x[:, c0 : c0 + sizes[p]], ins[p][...], preferred_element_type=F32)
            total = term if total is None else total + term
            c0 += sizes[p]
        o[...] = jnp.square(jnp.maximum(total, 0.0)).astype(BF)
        for c in copies:
            c.wait()

    in_specs = [SMEM] + [pl.BlockSpec((tok, width), lambda i: (0, 0))] * nb
    for p in pieces:
        first = j * steps if p.shape[1] == hid else 0
        in_specs.append(pl.BlockSpec((p.shape[0], sub), lambda i, f=first: (0, f + i)))
    args = [starts, *blocks, *pieces]
    aliases = {}
    if hidden is not None:
        in_specs += [ANY, ANY]
        args += [hidden, whole]
        aliases = {len(args) - 2: 0, len(args) - 1: 1}
    return pl.pallas_call(
        body,
        grid=(steps,),
        out_shape=(
            jax.ShapeDtypeStruct((n_tok, hid), BF),
            jax.ShapeDtypeStruct((rows, hid), BF),
        ),
        in_specs=in_specs,
        out_specs=(pl.BlockSpec((n_tok, sub), lambda i: (0, j * steps + i)), ANY),
        scratch_shapes=[pltpu.VMEM((n_tok, width), BF), pltpu.SemaphoreType.DMA((n,))],
        input_output_aliases=aliases,
        compiler_params=LIMIT,
        cost_estimate=pl.CostEstimate(
            flops=2 * n_tok * width * tile, bytes_accessed=4 * width * tile, transcendentals=0
        ),
        name="up_tile",
    )(*args)


def up_rest(block, whole, starts, sizes, sub=256):
    tok, width = block.shape
    hid = whole.shape[1]

    def body(at, x, w, o):
        total, c0 = None, 0
        for p, size in enumerate(sizes):
            rows = pl.ds(pl.multiple_of(at[p], 128), size)
            term = jnp.dot(x[:, c0 : c0 + size], w[rows, :], preferred_element_type=F32)
            total = term if total is None else total + term
            c0 += size
        o[...] = jnp.square(jnp.maximum(total, 0.0)).astype(BF)

    return pl.pallas_call(
        body,
        grid=(hid // sub,),
        out_shape=jax.ShapeDtypeStruct((tok, hid), BF),
        in_specs=[
            SMEM,
            pl.BlockSpec((tok, width), lambda i: (0, 0)),
            pl.BlockSpec((width, sub), lambda i: (0, i)),
        ],
        out_specs=pl.BlockSpec((tok, sub), lambda i: (0, i)),
        compiler_params=LIMIT,
        cost_estimate=pl.CostEstimate(
            flops=2 * tok * width * hid, bytes_accessed=2 * width * hid, transcendentals=0
        ),
        name="up_rest",
    )(starts, block, whole)


def down_step(hiddens, outs, pieces, starts, whole, rows, steps, keep_whole=True):
    hid = hiddens[0].shape[1]
    nh, n, no = len(hiddens), len(pieces), len(outs)
    sizes = [p.shape[0] // steps for p in pieces]
    cols = sum(sizes)
    n_tok = sum(h.shape[0] for h in hiddens)

    def body(*refs):
        at, hs, ins = refs[0], refs[1 : 1 + nh], refs[1 + nh : 1 + nh + n]
        tail = refs[-(no + 2) :] if keep_whole else refs[-no:]
        i = pl.program_id(0)
        copies = []
        if keep_whole:
            whole_out, sem = tail[no], tail[no + 1]
            for p in range(n):
                c = pltpu.make_async_copy(
                    ins[p],
                    whole_out.at[pl.ds(pl.multiple_of(at[p] + i * sizes[p], 16), sizes[p]), :],
                    sem.at[p],
                )
                c.start()
                copies.append(c)
        c0 = 0
        for p in range(n):
            prods = [
                lax.dot_general(
                    h[...], ins[p][...], (((1,), (1,)), ((), ())), preferred_element_type=F32
                ).astype(BF)
                for h in hs
            ]
            for o, runs in zip(tail, outs):
                r0 = 0
                for which, first, count in runs:
                    o[r0 : r0 + count, c0 : c0 + sizes[p]] = prods[which][first : first + count]
                    r0 += count
            c0 += sizes[p]
        for c in copies:
            c.wait()

    in_specs = [SMEM] + [pl.BlockSpec(h.shape, lambda i: (0, 0)) for h in hiddens]
    in_specs += [pl.BlockSpec((s, hid), lambda i: (i, 0)) for s in sizes]
    args = [starts, *hiddens, *pieces]
    out_shape, out_specs = [], []
    for runs in outs:
        count = sum(r[2] for r in runs)
        out_shape.append(jax.ShapeDtypeStruct((count, cols * steps), BF))
        out_specs.append(pl.BlockSpec((count, cols), lambda i: (0, i)))
    aliases, scratch = {}, []
    if keep_whole:
        out_shape.append(jax.ShapeDtypeStruct((rows, hid), BF))
        out_specs.append(ANY)
        scratch = [pltpu.SemaphoreType.DMA((n,))]
        if whole is not None:
            in_specs.append(ANY)
            args.append(whole)
            aliases = {len(args) - 1: no}
    return pl.pallas_call(
        body,
        grid=(steps,),
        out_shape=tuple(out_shape),
        in_specs=in_specs,
        out_specs=tuple(out_specs),
        scratch_shapes=scratch,
        input_output_aliases=aliases,
        compiler_params=LIMIT,
        cost_estimate=pl.CostEstimate(
            flops=2 * n_tok * cols * steps * hid,
            bytes_accessed=4 * cols * steps * hid + 2 * n_tok * hid,
            transcendentals=0,
        ),
        name="down_step",
    )(*args)


def finish(terms, starts, layout, post_gain, tok, width):
    counts = [len(t) for t in terms]

    def body(*refs):
        at, gain, ins, o = refs[0], refs[1], list(refs[2:-1]), refs[-1]
        sums = []
        for count in counts:
            group, ins = ins[:count], ins[count:]
            sums.append(sum(g[...].astype(F32) for g in group))
        power = sum(jnp.sum(s * s, axis=1, keepdims=True) for s in sums)
        scale = lax.rsqrt(power / width + 1e-06)
        for p, (i, c0, size) in enumerate(layout):
            to = pl.ds(pl.multiple_of(at[p], 128), size)
            o[:, to] = (sums[i][:, c0 : c0 + size] * scale * gain[:, to]).astype(BF)

    flat = [a for t in terms for a in t]
    vm = pl.BlockSpec(memory_space=pltpu.VMEM)
    return pl.pallas_call(
        body,
        grid=(1,),
        out_shape=jax.ShapeDtypeStruct((tok, width), BF),
        in_specs=[SMEM, pl.BlockSpec((1, width), lambda i: (0, 0))]
        + [pl.BlockSpec((tok, a.shape[1]), lambda i: (0, 0)) for a in flat],
        out_specs=pl.BlockSpec((tok, width), lambda i: (0, 0)),
        name="finish",
    )(starts, post_gain.reshape(1, width), *flat)


U_CUTS = 4
D_CUTS = 2


def routed(n_grp, n_fs, n_tp):
    n_y = n_fs // 2

    def grp_shift(v, d):
        return lax.ppermute(v, "grp", [((i + d) % n_grp, i) for i in range(n_grp)])

    def y_shift(v, d):
        return lax.ppermute(v, "fs", [((i + 2 * d) % n_fs, i) for i in range(n_fs)])

    def core_swap(v):
        return lax.ppermute(v, "fs", [(i, i ^ 1) for i in range(n_fs)])

    def tp_swap(v, m):
        return lax.ppermute(v, "tp", [(i, i ^ m) for i in range(n_tp)])

    def per_device(prompt_tokens, up_weight, down_weight, pre_gain, post_gain):
        fs = lax.axis_index("fs")
        grp = lax.axis_index("grp")
        rows, hid = up_weight.shape
        tok, width = prompt_tokens.shape
        half = rows // n_grp
        tile = hid // U_CUTS
        sub = half // D_CUTS

        def other(dy, dc):
            y = (fs // 2 + dy) % n_y
            return (2 * y + (fs % 2 if dc == 0 else 1 - fs % 2)) * rows

        def table(entries):
            return jnp.stack(entries).astype(jnp.int32)

        own_rows = [other(0, 0), other(0, 1)]
        sides = [((grp + j) % n_grp) * half for j in range(n_grp)]
        up_rows = own_rows + [other(1, dc) + s for dc in range(2) for s in sides]
        up_sizes = [rows, rows] + [half] * (2 * n_grp)
        up_at = table(up_rows)

        def exchange(mine):
            got = y_shift(mine, 1)
            near = [core_swap(got)]
            far = [got]
            for j in range(1, n_grp):
                part = grp_shift(got, j)
                far.append(part)
                near.append(core_swap(part))
            return far + near

        gain = pre_gain[:, None]
        half_up = lax.dynamic_slice_in_dim(up_weight, grp * half, half, 0)
        half_gain = lax.dynamic_slice_in_dim(gain, grp * half, half, 0)
        up_far = [
            exchange((half_up[:, i * tile : (i + 1) * tile] * half_gain).astype(BF))
            for i in range(U_CUTS)
        ]
        down_far = [
            exchange(lax.dynamic_slice_in_dim(down_weight, grp * half + i * sub, sub, 0).astype(BF))
            for i in range(D_CUTS)
        ]
        up_own = (up_weight * gain).astype(BF)
        up_near = [up_own, core_swap(up_own)]
        down_own = down_weight.astype(BF)
        down_near = [down_own, core_swap(down_own)]

        r0 = norm_tokens(prompt_tokens, up_at, up_sizes)
        r2 = tp_swap(r0, 2)
        r1 = tp_swap(r0, 1)
        r3 = tp_swap(r2, 1)

        hidden, whole_up = None, None
        for i in range(U_CUTS):
            hidden, whole_up = up_tile(
                [r1, r0, r2], up_near + up_far[i], up_at, i, U_CUTS, hidden, whole_up, n_fs * rows
            )
        hidden3 = up_rest(r3, whole_up, up_at, up_sizes)

        terms, layout, places = [], [], []

        def place(index, steps, starts, sizes):
            c0 = 0
            for j in range(steps):
                for start, size in zip(starts, sizes):
                    layout.append((index, c0, size // steps))
                    places.append(start + j * (size // steps))
                    c0 += size // steps

        near_steps = rows // 128
        near_at = table(own_rows)
        row1, row0, row2, row3 = (0, 0, tok), (0, tok, tok), (0, 2 * tok, tok), (1, 0, tok)
        send1, keep0, keep2, whole_down = down_step(
            [hidden], [[row1], [row0], [row2]], down_near, near_at, None, n_fs * rows, near_steps
        )
        got1 = tp_swap(send1, 1)
        (send3,) = down_step(
            [hidden3], [[(0, 0, tok)]], down_near, near_at, None, n_fs * rows, near_steps, False
        )
        got3 = tp_swap(send3, 1)
        pair = (keep2.astype(F32) + got3.astype(F32)).astype(BF)
        terms.append([keep0, got1, tp_swap(pair, 2)])
        place(0, near_steps, own_rows, [rows, rows])

        for i in range(D_CUTS):
            at = [other(1, dc) + s + i * sub for dc in range(2) for s in sides]
            send, keep0, keep2, whole_down = down_step(
                [hidden, hidden3],
                [[row1, row3], [row0], [row2]],
                down_far[i],
                table(at),
                whole_down,
                n_fs * rows,
                1,
            )
            got = tp_swap(send, 1)
            pair = (keep2.astype(F32) + got[tok:].astype(F32)).astype(BF)
            terms.append([keep0, got, tp_swap(pair, 2)])
            place(i + 1, 1, at, [sub] * len(at))
        mixed = finish(terms, table(places), layout, post_gain, tok, width)
        return mixed, whole_up, whole_down

    return per_device


def solution(mesh):
    n_grp, n_fs, n_tp = (mesh.shape[a] for a in ("grp", "fs", "tp"))
    placed = (P(("grp", "fs", "tp"), None), P("fs", "tp"), P("fs", "tp"), P("fs"), P())
    fits = n_grp == 2 and n_fs == 4 and n_tp == 4
    return jax.shard_map(
        routed(n_grp, n_fs, n_tp) if fits else plain,
        mesh=mesh,
        in_specs=placed,
        out_specs=(P(("grp", "fs", "tp"), None), P("grp", "tp"), P("grp", "tp")),
        check_vma=False,
    )
```

```python
import jax
import jax.numpy as jnp
from jax import lax
from jax.experimental import pallas as pl
from jax.experimental.pallas import tpu as pltpu
from jax.sharding import PartitionSpec as P


BF = jnp.bfloat16
F32 = jnp.float32
ANY = pl.BlockSpec(memory_space=pl.ANY)
LIMIT = pltpu.CompilerParams(vmem_limit_bytes=28 * 2**20)


def plain(prompt_tokens, up_weight, down_weight, pre_gain, post_gain):
    up_local = (up_weight * pre_gain[:, None]).astype(BF)
    down_local = down_weight.astype(BF)
    values = prompt_tokens.astype(F32)
    normed = (
        values * lax.rsqrt(jnp.mean(values * values, axis=1, keepdims=True) + 1e-06)
    ).astype(BF)
    sampler_up = lax.all_gather(up_local, "fs", axis=0, tiled=True)
    sampler_down = lax.all_gather(down_local, "fs", axis=0, tiled=True)
    lifted = jnp.dot(
        lax.all_gather(normed, "tp", axis=0, tiled=True),
        sampler_up,
        preferred_element_type=F32,
    )
    hidden = jnp.square(jax.nn.relu(lifted)).astype(BF)
    part = lax.dot_general(
        hidden, sampler_down, (((1,), (1,)), ((), ())), preferred_element_type=F32
    )
    summed = lax.psum_scatter(
        part.astype(BF), "tp", scatter_dimension=0, tiled=True
    ).astype(F32)
    scaled = summed * lax.rsqrt(jnp.mean(summed * summed, axis=1, keepdims=True) + 1e-06)
    return (scaled * post_gain[None, :]).astype(BF), sampler_up, sampler_down


def in_hbm(x):
    return pltpu.with_memory_space_constraint(x, pltpu.HBM)


def hbm_call(body, out_shape, args, **options):
    many = isinstance(out_shape, (tuple, list))
    return pl.pallas_call(
        body,
        out_shape=out_shape,
        in_specs=[ANY] * len(args),
        out_specs=tuple([ANY] * len(out_shape)) if many else ANY,
        **options,
    )(*args)


class Copies:
    def __init__(self, sems):
        self.sems, self.used = sems, 0

    def start(self, src, dst):
        c = pltpu.make_async_copy(src, dst, self.sems.at[self.used])
        self.used += 1
        c.start()
        return c


def wait_all(copies):
    for c in copies:
        c.wait()


def here():
    fs = lax.axis_index("fs")
    return fs // 2, fs % 2, lax.axis_index("grp")


def up_places(rows, half):
    y, core, grp = here()
    near = [(2 * y + core) * rows, (2 * y + 1 - core) * rows]
    far = [
        (2 * (1 - y) + c) * rows + side * half
        for c in (core, 1 - core)
        for side in (grp, 1 - grp)
    ]
    return [pl.multiple_of(a, 128) for a in near + far]


def cast(weight, gain, wanted, places, tokens=None, step=64):
    rows, hid = weight.shape
    n = len(wanted)
    whole = [w == (rows, hid) for w in wanted]
    parts = [(i, r) for i, w in enumerate(wanted) for r in range(0, w[0], step)]
    full = any(whole)
    if tokens is not None:
        tok, width = tokens.shape
        token_rows = [(r, tok // 2) for r in range(0, tok, tok // 2)]

    def body(*refs):
        w, refs = refs[0], refs[1:]
        if gain is not None:
            g, refs = refs[0], refs[1:]
        if tokens is not None:
            t, refs = refs[0], refs[1:]
        outs, refs = refs[:n], refs[n:]
        if tokens is not None:
            normed, refs = refs[0], refs[1:]
        src, bufs, refs = refs[0], refs[1 : 1 + n], refs[1 + n :]
        if gain is not None:
            line_in, column, refs = refs[0], refs[1], refs[2:]
        if tokens is not None:
            token_in, token_out, refs = refs[0], refs[1], refs[2:]
        go = Copies(refs[0])
        at = places()
        stores = []
        if gain is not None:
            line = go.start(g, line_in)

        if tokens is not None:
            token_loads = [
                go.start(t.at[r : r + c, :], token_in.at[r : r + c, :]) for r, c in token_rows
            ]

        def scaled(v, row, count):
            if gain is None:
                return v.astype(BF)
            return (v * column[pl.ds(row, count), :]).astype(BF)

        if full:
            loads = [
                go.start(w.at[r : r + step, :], src.at[r : r + step, :])
                for r in range(0, rows, step)
            ]
        else:
            loads = []
            for i, r in parts:
                row, col = at[i]
                loads.append(
                    go.start(
                        w.at[pl.ds(pl.multiple_of(row + r, 8), step), pl.ds(col, wanted[i][1])],
                        src.at[r : r + step, pl.ds(col, wanted[i][1])],
                    )
                )
        if gain is not None:
            line.wait()
            column[...] = jnp.broadcast_to(line_in[...], (128, rows)).T[:, :1]
        if tokens is not None:
            for load, (r, count) in zip(token_loads, token_rows):
                load.wait()
                v = token_in[r : r + count, :].astype(F32)
                token_out[r : r + count, :] = (
                    v * lax.rsqrt(jnp.mean(v * v, axis=1, keepdims=True) + 1e-06)
                ).astype(BF)
                stores.append(
                    go.start(token_out.at[r : r + count, :], normed.at[r : r + count, :])
                )
        if full:
            for k, r in enumerate(range(0, rows, step)):
                loads[k].wait()
                i = whole.index(True)
                bufs[i][r : r + step, :] = scaled(src[r : r + step, :], r, step)
                stores.append(go.start(bufs[i].at[r : r + step, :], outs[i].at[r : r + step, :]))
            for j in range(n):
                if not whole[j]:
                    row, col = at[j]
                    stores.append(
                        go.start(
                            bufs[i].at[
                                pl.ds(pl.multiple_of(row, 16), wanted[j][0]),
                                pl.ds(col, wanted[j][1]),
                            ],
                            outs[j],
                        )
                    )
        else:
            for k, (i, r) in enumerate(parts):
                row, col = at[i]
                loads[k].wait()
                bufs[i][r : r + step, :] = scaled(
                    src[r : r + step, col : col + wanted[i][1]], row + r, step
                )
                stores.append(go.start(bufs[i].at[r : r + step, :], outs[i].at[r : r + step, :]))
        wait_all(stores)

    out_shape = [jax.ShapeDtypeStruct(w, BF) for w in wanted]
    scratch = [pltpu.VMEM((rows, hid) if n else (8, 128), F32)]
    scratch += [pltpu.VMEM(w, BF) for w in wanted]
    args = [in_hbm(weight)]
    if gain is not None:
        args.append(in_hbm(gain))
        scratch += [pltpu.VMEM((1, rows), F32), pltpu.VMEM((rows, 1), F32)]
    if tokens is not None:
        args.append(in_hbm(tokens))
        out_shape.append(jax.ShapeDtypeStruct((tok, width), BF))
        scratch += [pltpu.VMEM((tok, width), BF), pltpu.VMEM((tok, width), BF)]
    n_sem = 2 * rows // step + n + 2 * len(parts) + 8
    return hbm_call(
        body,
        tuple(out_shape),
        args,
        scratch_shapes=scratch + [pltpu.SemaphoreType.DMA((n_sem,))],
        compiler_params=LIMIT,
        cost_estimate=pl.CostEstimate(
            flops=10**8, bytes_accessed=6 * rows * hid, transcendentals=0
        ),
        name="cast",
    )


def feed(blocks, near, chunks, prev, down_near, cuts, n_chunk=512):
    tok, width = blocks[0].shape
    rows, hid = near[0].shape
    half = rows // 2
    tile = chunks[0][1][0].shape[1]
    nb, nc, npv = len(blocks), len(chunks), len(prev)
    n_tok = nb * tok
    nf = len(chunks[0][1])
    n_in = nb + 2 + nc * nf + npv + (2 if down_near else 0)
    n_out = nc + (len(cuts) if down_near else 0)
    n_sem = n_in + nc * 2 + n_out * (2 * rows // n_chunk + 1)

    def body(*refs):
        ins, outs, scratch = refs[:n_in], refs[n_in : n_in + n_out], refs[n_in + n_out :]
        x, w, h, sems = scratch[0], scratch[1], scratch[2], scratch[-1]
        go = Copies(sems)
        tok_in, ins = ins[:nb], ins[nb:]
        near_in, ins = ins[:2], ins[2:]
        loads = [go.start(tok_in[b], x.at[b * tok : (b + 1) * tok, :]) for b in range(nb)]
        at = up_places(rows, half)
        per_tile = []
        for k, (t, _) in enumerate(chunks):
            far, ins = ins[:nf], ins[nf:]
            cols = pl.ds(t * tile, tile)
            srcs = [a.at[:, cols] for a in near_in] + list(far)
            sizes = [rows, rows] + [half] * nf
            per_tile.append(
                [
                    go.start(src, w.at[k, pl.ds(a, size), :])
                    for src, a, size in zip(srcs, at, sizes)
                ]
            )
        late = [go.start(ins[i], h.at[:, i * tile : (i + 1) * tile]) for i in range(npv)]
        ins = ins[npv:]
        if down_near:
            d, o = scratch[3], scratch[4]
            core = here()[1]
            late.append(go.start(ins[0], d.at[pl.ds(pl.multiple_of(core * rows, 128), rows), :]))
            late.append(
                go.start(ins[1], d.at[pl.ds(pl.multiple_of((1 - core) * rows, 128), rows), :])
            )
        wait_all(loads)
        stores = []
        for k, (t, _) in enumerate(chunks):
            wait_all(per_tile[k])
            for c in range(0, tile, n_chunk):
                n = min(n_chunk, tile)
                lifted = jnp.dot(x[...], w[k, :, c : c + n], preferred_element_type=F32)
                h[:, t * tile + c : t * tile + c + n] = jnp.square(
                    jnp.maximum(lifted, 0.0)
                ).astype(BF)
            stores.append(go.start(h.at[:, t * tile : (t + 1) * tile], outs[k]))
        wait_all(late)
        if down_near:
            for c in range(0, 2 * rows, n_chunk):
                o[:, c : c + n_chunk] = lax.dot_general(
                    h[...],
                    d[c : c + n_chunk, :],
                    (((1,), (1,)), ((), ())),
                    preferred_element_type=F32,
                ).astype(BF)
                for out, (first, count) in zip(outs[nc:], cuts):
                    stores.append(
                        go.start(
                            o.at[first : first + count, c : c + n_chunk],
                            out.at[:, c : c + n_chunk],
                        )
                    )
        wait_all(stores)

    out_shape = [jax.ShapeDtypeStruct((n_tok, tile), BF)] * nc
    scratch = [
        pltpu.VMEM((n_tok, width), BF),
        pltpu.VMEM((nc, width, tile), BF),
        pltpu.VMEM((n_tok, hid), BF),
    ]
    flops = 2 * n_tok * width * tile * nc
    if down_near:
        out_shape += [jax.ShapeDtypeStruct((count, 2 * rows), BF) for _, count in cuts]
        scratch += [pltpu.VMEM((2 * rows, hid), BF), pltpu.VMEM((n_tok, 2 * rows), BF)]
        flops += 2 * n_tok * hid * 2 * rows
    args = list(blocks) + list(near)
    for _, far in chunks:
        args += far
    args += list(prev) + list(down_near or [])
    return hbm_call(
        body,
        tuple(out_shape),
        args,
        scratch_shapes=scratch + [pltpu.SemaphoreType.DMA((n_sem,))],
        compiler_params=LIMIT,
        cost_estimate=pl.CostEstimate(
            flops=flops, bytes_accessed=2 * width * tile * nc, transcendentals=0
        ),
        name="feed",
    )


def down_far_step(hiddens, groups, cuts, sub):
    hid = groups[0][0].shape[1]
    n_groups, nf = len(groups), len(groups[0])
    counts = [h[0].shape[0] for h in hiddens]
    n_tok = sum(counts)
    n_h = sum(len(h) for h in hiddens)
    cols = n_groups * nf * sub
    n_in = n_h + n_groups * nf

    def body(*refs):
        ins, outs = refs[:n_in], refs[n_in : n_in + len(cuts)]
        h, d, o, sems = refs[n_in + len(cuts) :]
        go = Copies(sems)
        loads, k, r0 = [], 0, 0
        for tiles, count in zip(hiddens, counts):
            c0 = 0
            for t in tiles:
                loads.append(go.start(ins[k], h.at[r0 : r0 + count, c0 : c0 + t.shape[1]]))
                c0 += t.shape[1]
                k += 1
            r0 += count
        _, core, grp = here()
        for g in range(n_groups):
            place = [
                c * (cols // 2) + g * 2 * sub + side * sub
                for c in (core, 1 - core)
                for side in (grp, 1 - grp)
            ]
            for a in place:
                loads.append(go.start(ins[k], d.at[pl.ds(pl.multiple_of(a, 64), sub), :]))
                k += 1
        wait_all(loads)
        o[...] = lax.dot_general(
            h[...], d[...], (((1,), (1,)), ((), ())), preferred_element_type=F32
        ).astype(BF)
        stores = []
        for out, runs in zip(outs, cuts):
            r0 = 0
            for first, count in runs:
                stores.append(
                    go.start(o.at[first : first + count, :], out.at[r0 : r0 + count, :])
                )
                r0 += count
        wait_all(stores)

    return hbm_call(
        body,
        tuple(jax.ShapeDtypeStruct((sum(c for _, c in runs), cols), BF) for runs in cuts),
        [t for h in hiddens for t in h] + [p for g in groups for p in g],
        scratch_shapes=[
            pltpu.VMEM((n_tok, hid), BF),
            pltpu.VMEM((cols, hid), BF),
            pltpu.VMEM((n_tok, cols), BF),
            pltpu.SemaphoreType.DMA((n_in + sum(len(r) for r in cuts),)),
        ],
        compiler_params=LIMIT,
        cost_estimate=pl.CostEstimate(
            flops=2 * n_tok * cols * hid, bytes_accessed=2 * cols * hid, transcendentals=0
        ),
        name="down_far",
    )


def assemble(near, far, shape, places):
    pieces = list(near) + [p for g in far for p in g]

    def body(*refs):
        ins, out, buf, sems = refs[: len(pieces)], refs[len(pieces)], refs[-2], refs[-1]
        go = Copies(sems)
        spots = [
            (pl.ds(row, p.shape[0]), pl.ds(col, p.shape[1]))
            for p, (row, col) in zip(pieces, places())
        ]
        loads = [go.start(ref, buf.at[spot]) for ref, spot in zip(ins, spots)]
        stores = []
        for load, spot in zip(loads, spots):
            load.wait()
            stores.append(go.start(buf.at[spot], out.at[spot]))
        wait_all(stores)

    return hbm_call(
        body,
        jax.ShapeDtypeStruct(shape, BF),
        pieces,
        scratch_shapes=[pltpu.VMEM(shape, BF), pltpu.SemaphoreType.DMA((2 * len(pieces),))],
        compiler_params=LIMIT,
        cost_estimate=pl.CostEstimate(
            flops=10**9, bytes_accessed=4 * shape[0] * shape[1], transcendentals=0
        ),
        name="assemble",
    )


def add_rows(keep, got):
    return (keep.astype(F32) + got.astype(F32)).astype(BF)


def finish(near, far, post_gain, tok, rows):
    width = 4 * rows
    terms = [near] + far
    flat = [a for t in terms for a in t]

    def body(*refs):
        gain, ins, o = refs[0], list(refs[1:-1]), refs[-1]
        sums = []
        for t in terms:
            group, ins = ins[: len(t)], ins[len(t) :]
            sums.append(sum(g[:tok].astype(F32) for g in group))
        power = sum(jnp.sum(s * s, axis=1, keepdims=True) for s in sums)
        scale = lax.rsqrt(power / width + 1e-06)
        y = here()[0]

        def put(value, start):
            to = pl.ds(pl.multiple_of(start, 128), value.shape[1])
            o[:, to] = (value * scale * gain[:, to]).astype(BF)

        put(sums[0], y * 2 * rows)
        c0 = 0
        for s in sums[1:]:
            n = s.shape[1] // 2
            for c in range(2):
                put(s[:, c * n : (c + 1) * n], (1 - y) * 2 * rows + c * rows + c0)
            c0 += n

    vm = pl.BlockSpec(memory_space=pltpu.VMEM)
    return pl.pallas_call(
        body,
        out_shape=jax.ShapeDtypeStruct((tok, width), BF),
        in_specs=[vm] * (1 + len(flat)),
        out_specs=vm,
        name="finish",
    )(post_gain.reshape(1, width), *flat)


U_CUTS = 4
D_CUTS = 4
LEAD = 3
ROUNDS = ((0, 1), (2, 3))


def routed():
    def grp_swap(v):
        return lax.ppermute(v, "grp", [(0, 1), (1, 0)])

    def y_swap(v):
        return lax.ppermute(v, "fs", [(i, i ^ 2) for i in range(4)])

    def core_swap(v):
        return lax.ppermute(v, "fs", [(i, i ^ 1) for i in range(4)])

    def tp_swap(v, m):
        return lax.ppermute(v, "tp", [(i, i ^ m) for i in range(4)])

    def per_device(prompt_tokens, up_weight, down_weight, pre_gain, post_gain):
        rows, hid = up_weight.shape
        tok, _ = prompt_tokens.shape
        half = rows // 2
        tile = hid // U_CUTS
        sub = half // D_CUTS

        def exchange(mine):
            got = y_swap(mine)
            near = core_swap(got)
            part = grp_swap(got)
            return [got, part, near, core_swap(part)]

        gain = pre_gain.reshape(1, rows)
        spots = [lambda i=i: (here()[2] * half, i * tile) for i in range(U_CUTS)]
        block = (half, tile)
        lead = cast(up_weight, gain, [block] * LEAD, lambda: [f() for f in spots[:LEAD]])
        *_, r0 = cast(up_weight, None, [], lambda: [], prompt_tokens)
        up_own, *rest = cast(
            up_weight,
            gain,
            [(rows, hid)] + [block] * (U_CUTS - LEAD),
            lambda: [(0, 0)] + [f() for f in spots[LEAD:]],
        )
        down_own, *mine = cast(
            down_weight,
            None,
            [(rows, hid)] + [(sub, hid)] * D_CUTS,
            lambda: [(0, 0)] + [((2 * i + here()[2]) * sub, 0) for i in range(D_CUTS)],
        )
        up_far = [exchange(v) for v in [*lead, *rest]]
        down_far = [exchange(v) for v in mine]
        up_near = [up_own, core_swap(up_own)]
        down_near = [down_own, core_swap(down_own)]

        r2 = tp_swap(r0, 2)
        r1 = tp_swap(r0, 1)
        r3 = tp_swap(r2, 1)

        tiles = list(enumerate(up_far))
        cut = [(0, tok), (tok, tok), (2 * tok, tok)]
        hidden = list(feed([r1, r0, r2], up_near, tiles[:-1], [], None, []))
        last, send1, keep0, keep2 = feed([r1, r0, r2], up_near, tiles[-1:], hidden, down_near, cut)
        hidden = hidden + [last]
        got1 = tp_swap(send1, 1)
        *hidden3, send3 = feed([r3], up_near, tiles, [], down_near, cut[:1])
        got3 = tp_swap(send3, 1)
        pair = add_rows(keep2, got3)
        near_terms = [keep0, got1, tp_swap(pair, 2)]

        far_terms = []
        cuts = [[cut[0], (3 * tok, tok)], [cut[1]], [cut[2]]]
        for ids in ROUNDS:
            send, keep0, keep2 = down_far_step(
                [hidden, hidden3], [down_far[g] for g in ids], cuts, sub
            )
            got = tp_swap(send, 1)
            pair = add_rows(keep2, got[tok:])
            far_terms.append([keep0, got, tp_swap(pair, 2)])

        def up_spots():
            at = up_places(rows, half)
            spots = [(a, 0) for a in at[:2]]
            return spots + [(a, i * tile) for i in range(U_CUTS) for a in at[2:]]

        def down_spots():
            y, core, grp = here()
            spots = [((2 * y + c) * rows, 0) for c in (core, 1 - core)]
            for i in range(D_CUTS):
                spots += [
                    ((2 * (1 - y) + c) * rows + (2 * i + side) * sub, 0)
                    for c in (core, 1 - core)
                    for side in (grp, 1 - grp)
                ]
            return [(pl.multiple_of(a, 64), c) for a, c in spots]

        shape = (4 * rows, hid)
        whole_up = assemble(up_near, up_far, shape, up_spots)
        whole_down = assemble(down_near, down_far, shape, down_spots)
        mixed = finish(near_terms, far_terms, post_gain, tok, rows)
        return mixed, whole_up, whole_down

    return per_device


def solution(mesh):
    placed = (P(("grp", "fs", "tp"), None), P("fs", "tp"), P("fs", "tp"), P("fs"), P())
    fits = all(mesh.shape[a] == n for a, n in (("grp", 2), ("fs", 4), ("tp", 4)))
    return jax.shard_map(
        routed() if fits else plain,
        mesh=mesh,
        in_specs=placed,
        out_specs=(P(("grp", "fs", "tp"), None), P("grp", "tp"), P("grp", "tp")),
        check_vma=False,
    )
```

```python
import jax
import jax.numpy as jnp
from jax import lax
from jax.experimental import pallas as pl
from jax.experimental.pallas import tpu as pltpu
from jax.sharding import PartitionSpec as P


BF = jnp.bfloat16
F32 = jnp.float32
ANY = pl.BlockSpec(memory_space=pl.ANY)
LIMIT = pltpu.CompilerParams(vmem_limit_bytes=28 * 2**20)


def plain(prompt_tokens, up_weight, down_weight, pre_gain, post_gain):
    up_local = (up_weight * pre_gain[:, None]).astype(BF)
    down_local = down_weight.astype(BF)
    values = prompt_tokens.astype(F32)
    normed = (
        values * lax.rsqrt(jnp.mean(values * values, axis=1, keepdims=True) + 1e-06)
    ).astype(BF)
    sampler_up = lax.all_gather(up_local, "fs", axis=0, tiled=True)
    sampler_down = lax.all_gather(down_local, "fs", axis=0, tiled=True)
    lifted = jnp.dot(
        lax.all_gather(normed, "tp", axis=0, tiled=True),
        sampler_up,
        preferred_element_type=F32,
    )
    hidden = jnp.square(jax.nn.relu(lifted)).astype(BF)
    part = lax.dot_general(
        hidden, sampler_down, (((1,), (1,)), ((), ())), preferred_element_type=F32
    )
    summed = lax.psum_scatter(
        part.astype(BF), "tp", scatter_dimension=0, tiled=True
    ).astype(F32)
    scaled = summed * lax.rsqrt(jnp.mean(summed * summed, axis=1, keepdims=True) + 1e-06)
    return (scaled * post_gain[None, :]).astype(BF), sampler_up, sampler_down


def in_hbm(x):
    return pltpu.with_memory_space_constraint(x, pltpu.HBM)


def in_vmem(x):
    return pltpu.with_memory_space_constraint(x, pltpu.VMEM)


def hbm_call(body, out_shape, args, **options):
    many = isinstance(out_shape, (tuple, list))
    return pl.pallas_call(
        body,
        out_shape=out_shape,
        in_specs=[ANY] * len(args),
        out_specs=tuple([ANY] * len(out_shape)) if many else ANY,
        **options,
    )(*args)


class Copies:
    def __init__(self, sems):
        self.sems, self.used = sems, 0

    def start(self, src, dst):
        c = pltpu.make_async_copy(src, dst, self.sems.at[self.used])
        self.used += 1
        c.start()
        return c


def wait_all(copies):
    for c in copies:
        c.wait()


def here():
    fs = lax.axis_index("fs")
    return fs // 2, fs % 2, lax.axis_index("grp")


def up_places(rows, half):
    y, core, grp = here()
    near = [(2 * y + core) * rows, (2 * y + 1 - core) * rows]
    far = [
        (2 * (1 - y) + c) * rows + side * half
        for c in (core, 1 - core)
        for side in (grp, 1 - grp)
    ]
    return [pl.multiple_of(a, 128) for a in near + far]


def cast(weight, gain, wanted, places, tokens=None, step=64):
    rows, hid = weight.shape
    n = len(wanted)
    whole = [w == (rows, hid) for w in wanted]
    parts = [(i, r) for i, w in enumerate(wanted) for r in range(0, w[0], step)]
    full = any(whole)
    if tokens is not None:
        tok, width = tokens.shape
        token_rows = [(r, tok // 2) for r in range(0, tok, tok // 2)]

    def body(*refs):
        w, refs = refs[0], refs[1:]
        if gain is not None:
            g, refs = refs[0], refs[1:]
        if tokens is not None:
            t, refs = refs[0], refs[1:]
        outs, refs = refs[:n], refs[n:]
        if tokens is not None:
            normed, refs = refs[0], refs[1:]
        src, bufs, refs = refs[0], refs[1 : 1 + n], refs[1 + n :]
        if gain is not None:
            line_in, column, refs = refs[0], refs[1], refs[2:]
        if tokens is not None:
            token_in, token_out, refs = refs[0], refs[1], refs[2:]
        go = Copies(refs[0])
        at = places()
        stores = []
        if gain is not None:
            line = go.start(g, line_in)

        if tokens is not None:
            token_loads = [
                go.start(t.at[r : r + c, :], token_in.at[r : r + c, :]) for r, c in token_rows
            ]

        def scaled(v, row, count):
            if gain is None:
                return v.astype(BF)
            return (v * column[pl.ds(row, count), :]).astype(BF)

        if full:
            loads = [
                go.start(w.at[r : r + step, :], src.at[r : r + step, :])
                for r in range(0, rows, step)
            ]
        else:
            loads = []
            for i, r in parts:
                row, col = at[i]
                loads.append(
                    go.start(
                        w.at[pl.ds(pl.multiple_of(row + r, 8), step), pl.ds(col, wanted[i][1])],
                        src.at[r : r + step, pl.ds(col, wanted[i][1])],
                    )
                )
        if gain is not None:
            line.wait()
            column[...] = jnp.broadcast_to(line_in[...], (128, rows)).T[:, :1]
        if tokens is not None:
            for load, (r, count) in zip(token_loads, token_rows):
                load.wait()
                v = token_in[r : r + count, :].astype(F32)
                token_out[r : r + count, :] = (
                    v * lax.rsqrt(jnp.mean(v * v, axis=1, keepdims=True) + 1e-06)
                ).astype(BF)
                stores.append(
                    go.start(token_out.at[r : r + count, :], normed.at[r : r + count, :])
                )
        if full:
            for k, r in enumerate(range(0, rows, step)):
                loads[k].wait()
                i = whole.index(True)
                bufs[i][r : r + step, :] = scaled(src[r : r + step, :], r, step)
                stores.append(go.start(bufs[i].at[r : r + step, :], outs[i].at[r : r + step, :]))
            for j in range(n):
                if not whole[j]:
                    row, col = at[j]
                    stores.append(
                        go.start(
                            bufs[i].at[
                                pl.ds(pl.multiple_of(row, 16), wanted[j][0]),
                                pl.ds(col, wanted[j][1]),
                            ],
                            outs[j],
                        )
                    )
        else:
            for k, (i, r) in enumerate(parts):
                row, col = at[i]
                loads[k].wait()
                bufs[i][r : r + step, :] = scaled(
                    src[r : r + step, col : col + wanted[i][1]], row + r, step
                )
                stores.append(go.start(bufs[i].at[r : r + step, :], outs[i].at[r : r + step, :]))
        wait_all(stores)

    out_shape = [jax.ShapeDtypeStruct(w, BF) for w in wanted]
    scratch = [pltpu.VMEM((rows, hid) if n else (8, 128), F32)]
    scratch += [pltpu.VMEM(w, BF) for w in wanted]
    args = [in_hbm(weight)]
    if gain is not None:
        args.append(in_hbm(gain))
        scratch += [pltpu.VMEM((1, rows), F32), pltpu.VMEM((rows, 1), F32)]
    if tokens is not None:
        args.append(in_hbm(tokens))
        out_shape.append(jax.ShapeDtypeStruct((tok, width), BF))
        scratch += [pltpu.VMEM((tok, width), BF), pltpu.VMEM((tok, width), BF)]
    n_sem = 2 * rows // step + n + 2 * len(parts) + 8
    return hbm_call(
        body,
        tuple(out_shape),
        args,
        scratch_shapes=scratch + [pltpu.SemaphoreType.DMA((n_sem,))],
        compiler_params=LIMIT,
        cost_estimate=pl.CostEstimate(
            flops=10**8, bytes_accessed=6 * rows * hid, transcendentals=0
        ),
        name="cast",
    )


def feed(blocks, near, chunks, prev, down_near, cuts, n_chunk=512):
    tok, width = blocks[0].shape
    rows, hid = near[0].shape
    half = rows // 2
    tile = chunks[0][1][0].shape[1]
    nb, nc, npv = len(blocks), len(chunks), len(prev)
    n_tok = nb * tok
    nf = len(chunks[0][1])
    n_in = nb + 2 + nc * nf + npv + (2 if down_near else 0)
    n_out = nc + (len(cuts) if down_near else 0)
    n_sem = n_in + nc * 2 + n_out * (2 * rows // n_chunk + 1)

    def body(*refs):
        ins, outs, scratch = refs[:n_in], refs[n_in : n_in + n_out], refs[n_in + n_out :]
        x, w, h, sems = scratch[0], scratch[1], scratch[2], scratch[-1]
        go = Copies(sems)
        tok_in, ins = ins[:nb], ins[nb:]
        near_in, ins = ins[:2], ins[2:]
        loads = [go.start(tok_in[b], x.at[b * tok : (b + 1) * tok, :]) for b in range(nb)]
        at = up_places(rows, half)
        per_tile = []
        for k, (t, _) in enumerate(chunks):
            far, ins = ins[:nf], ins[nf:]
            cols = pl.ds(t * tile, tile)
            srcs = [a.at[:, cols] for a in near_in] + list(far)
            sizes = [rows, rows] + [half] * nf
            per_tile.append(
                [
                    go.start(src, w.at[k, pl.ds(a, size), :])
                    for src, a, size in zip(srcs, at, sizes)
                ]
            )
        late = [go.start(ins[i], h.at[:, i * tile : (i + 1) * tile]) for i in range(npv)]
        ins = ins[npv:]
        if down_near:
            d, o = scratch[3], scratch[4]
            core = here()[1]
            late.append(go.start(ins[0], d.at[pl.ds(pl.multiple_of(core * rows, 128), rows), :]))
            late.append(
                go.start(ins[1], d.at[pl.ds(pl.multiple_of((1 - core) * rows, 128), rows), :])
            )
        wait_all(loads)
        stores = []
        for k, (t, _) in enumerate(chunks):
            wait_all(per_tile[k])
            for c in range(0, tile, n_chunk):
                n = min(n_chunk, tile)
                lifted = jnp.dot(x[...], w[k, :, c : c + n], preferred_element_type=F32)
                h[:, t * tile + c : t * tile + c + n] = jnp.square(
                    jnp.maximum(lifted, 0.0)
                ).astype(BF)
            stores.append(go.start(h.at[:, t * tile : (t + 1) * tile], outs[k]))
        wait_all(late)
        if down_near:
            for c in range(0, 2 * rows, n_chunk):
                o[:, c : c + n_chunk] = lax.dot_general(
                    h[...],
                    d[c : c + n_chunk, :],
                    (((1,), (1,)), ((), ())),
                    preferred_element_type=F32,
                ).astype(BF)
                for out, (first, count) in zip(outs[nc:], cuts):
                    stores.append(
                        go.start(
                            o.at[first : first + count, c : c + n_chunk],
                            out.at[:, c : c + n_chunk],
                        )
                    )
        wait_all(stores)

    out_shape = [jax.ShapeDtypeStruct((n_tok, tile), BF)] * nc
    scratch = [
        pltpu.VMEM((n_tok, width), BF),
        pltpu.VMEM((nc, width, tile), BF),
        pltpu.VMEM((n_tok, hid), BF),
    ]
    flops = 2 * n_tok * width * tile * nc
    if down_near:
        out_shape += [
            pltpu.HBM((count, 2 * rows), BF)
            if i == 1
            else jax.ShapeDtypeStruct((count, 2 * rows), BF)
            for i, (_, count) in enumerate(cuts)
        ]
        scratch += [pltpu.VMEM((2 * rows, hid), BF), pltpu.VMEM((n_tok, 2 * rows), BF)]
        flops += 2 * n_tok * hid * 2 * rows
    args = list(blocks) + list(near)
    for _, far in chunks:
        args += far
    args += list(prev) + list(down_near or [])
    return hbm_call(
        body,
        tuple(out_shape),
        args,
        scratch_shapes=scratch + [pltpu.SemaphoreType.DMA((n_sem,))],
        compiler_params=LIMIT,
        cost_estimate=pl.CostEstimate(
            flops=flops, bytes_accessed=2 * width * tile * nc, transcendentals=0
        ),
        name="feed",
    )


def down_far_step(hiddens, groups, cuts, sub, before):
    hid = groups[0][0].shape[1]
    n_groups, nf = len(groups), len(groups[0])
    counts = [h[0].shape[0] for h in hiddens]
    n_tok = sum(counts)
    n_h = sum(len(h) for h in hiddens)
    cols = n_groups * nf * sub
    ahead = 0 if before is None else before.shape[1]
    n_in = n_h + n_groups * nf + (ahead > 0)

    def body(*refs):
        ins, outs = refs[:n_in], refs[n_in : n_in + len(cuts)]
        h, d, o, sems = refs[n_in + len(cuts) :]
        go = Copies(sems)
        loads, k, r0 = [], 0, 0
        for tiles, count in zip(hiddens, counts):
            c0 = 0
            for t in tiles:
                loads.append(go.start(ins[k], h.at[r0 : r0 + count, c0 : c0 + t.shape[1]]))
                c0 += t.shape[1]
                k += 1
            r0 += count
        _, core, grp = here()
        for g in range(n_groups):
            place = [
                c * (cols // 2) + g * 2 * sub + side * sub
                for c in (core, 1 - core)
                for side in (grp, 1 - grp)
            ]
            for a in place:
                loads.append(go.start(ins[k], d.at[pl.ds(pl.multiple_of(a, 64), sub), :]))
                k += 1
        stores = []
        if ahead:
            stores.append(go.start(ins[k], outs[-1].at[:, :ahead]))
        wait_all(loads)
        o[...] = lax.dot_general(
            h[...], d[...], (((1,), (1,)), ((), ())), preferred_element_type=F32
        ).astype(BF)
        for q, (out, runs) in enumerate(zip(outs, cuts)):
            r0 = 0
            for first, count in runs:
                to = pl.ds(ahead if q == len(cuts) - 1 else 0, cols)
                stores.append(
                    go.start(o.at[first : first + count, :], out.at[r0 : r0 + count, to])
                )
                r0 += count
        wait_all(stores)

    return hbm_call(
        body,
        tuple(
            (pltpu.HBM if i == 1 else jax.ShapeDtypeStruct)(
                (sum(c for _, c in runs), cols + (ahead if i == len(cuts) - 1 else 0)), BF
            )
            for i, runs in enumerate(cuts)
        ),
        [t for h in hiddens for t in h]
        + [p for g in groups for p in g]
        + ([before] if ahead else []),
        scratch_shapes=[
            pltpu.VMEM((n_tok, hid), BF),
            pltpu.VMEM((cols, hid), BF),
            pltpu.VMEM((n_tok, cols), BF),
            pltpu.SemaphoreType.DMA((n_in + sum(len(r) for r in cuts),)),
        ],
        compiler_params=LIMIT,
        cost_estimate=pl.CostEstimate(
            flops=2 * n_tok * cols * hid, bytes_accessed=2 * cols * hid, transcendentals=0
        ),
        name="down_far",
    )


def assemble(pieces, shape, places, base=None):
    n = len(pieces)

    def body(*refs):
        ins, out, buf, sems = refs[:n], refs[-3], refs[-2], refs[-1]
        go = Copies(sems)
        spots = [
            (pl.ds(row, p.shape[0]), pl.ds(col, p.shape[1]))
            for p, (row, col) in zip(pieces, places())
        ]
        spaces, at = [], 0
        for p in pieces:
            spaces.append(buf.at[at : at + p.shape[0], : p.shape[1]])
            at += p.shape[0]
        loads = [go.start(ref, space) for ref, space in zip(ins, spaces)]
        stores = []
        for load, space, spot in zip(loads, spaces, spots):
            load.wait()
            stores.append(go.start(space, out.at[spot]))
        wait_all(stores)

    args = list(pieces) + ([base] if base is not None else [])
    total = sum(p.shape[0] for p in pieces)
    return hbm_call(
        body,
        jax.ShapeDtypeStruct(shape, BF),
        args,
        input_output_aliases={n: 0} if base is not None else {},
        scratch_shapes=[
            pltpu.VMEM((total, max(p.shape[1] for p in pieces)), BF),
            pltpu.SemaphoreType.DMA((2 * n,)),
        ],
        compiler_params=LIMIT,
        cost_estimate=pl.CostEstimate(
            flops=10**9, bytes_accessed=2 * shape[0] * shape[1], transcendentals=0
        ),
        name="assemble",
    )


def add_rows(keep, got):
    return (keep.astype(F32) + got.astype(F32)).astype(BF)


def before_last(near, far, post_gain, rows):
    width = 4 * rows
    terms = [near] + far
    flat = [a for t in terms for a in t]
    tok = near[0].shape[0]
    counts = [t[0].shape[1] for t in terms]
    n_far = sum(counts[1:])

    def body(*refs):
        n_in = 1 + len(flat)
        o, part, part_gain, power = refs[n_in : n_in + 4]
        local, sems = refs[n_in + 4 : -1], refs[-1]
        go = Copies(sems)
        wait_all([go.start(a.at[: b.shape[0]], b) for a, b in zip(refs[:n_in], local)])
        gain, ins = local[0], list(local[1:])
        sums = []
        for t in terms:
            group, ins = ins[: len(t)], ins[len(t) :]
            sums.append(sum(g[...].astype(F32) for g in group))
        total = jnp.sum(sums[0] * sums[0], axis=1, keepdims=True)
        power[...] = jnp.broadcast_to(total, (tok, 128))
        at = 0
        for s in sums[1:]:
            part[:, at : at + s.shape[1]] = s
            at += s.shape[1]
        for y in range(2):

            @pl.when(here()[0] == y)
            def _(y=y):
                place = near_place(y, rows)
                o[:, place] = sums[0] * gain[:, place]
                for place, at, n in far_places(y, rows, counts[1:]):
                    part_gain[:, at : at + n] = gain[:, place]

    vm = pl.BlockSpec(memory_space=pltpu.VMEM)
    return pl.pallas_call(
        body,
        out_shape=(
            pltpu.VMEM((tok, width), F32),
            pltpu.VMEM((tok, n_far), F32),
            pltpu.VMEM((1, n_far), F32),
            pltpu.VMEM((tok, 128), F32),
        ),
        in_specs=[ANY] * (1 + len(flat)),
        out_specs=(vm,) * 4,
        scratch_shapes=[pltpu.VMEM((1, width), F32)]
        + [pltpu.VMEM((tok, a.shape[1]), BF) for a in flat]
        + [pltpu.SemaphoreType.DMA((1 + len(flat),))],
        name="before_last",
    )(post_gain.reshape(1, width), *flat)


def near_place(y, rows):
    return slice(y * 2 * rows, (y + 1) * 2 * rows)


def far_places(y, rows, counts):
    found, at, before = [], 0, 0
    for count in counts:
        n = count // 2
        for c in range(2):
            start = (1 - y) * 2 * rows + c * rows + before
            found.append((slice(start, start + n), at, n))
            at += n
        before += n
    return found


def finish(ready, part, part_gain, power, one, two, counts, rows):
    tok, width = ready.shape
    n_two = two.shape[1]

    def body(r, p, g, w, a, b, out, v, o, sems):
        v[...] = p[...] + a[...].astype(F32)
        v[:, -n_two:] += b[...].astype(F32)
        total = w[:, :1] + jnp.sum(v[...] * v[...], axis=1, keepdims=True)
        scale = lax.rsqrt(total / width + 1e-06)
        go = Copies(sems)
        step = tok // 4
        stores = []
        for r0 in range(0, tok, step):
            own = slice(r0, r0 + step)
            for y in range(2):

                @pl.when(here()[0] == y)
                def _(y=y):
                    place = near_place(y, rows)
                    o[own, place] = (r[own, place] * scale[own]).astype(BF)
                    for place, at, n in far_places(y, rows, counts):
                        cols = slice(at, at + n)
                        o[own, place] = (v[own, cols] * g[:, cols] * scale[own]).astype(BF)

            stores.append(go.start(o.at[own, :], out.at[own, :]))
        wait_all(stores)

    vm = pl.BlockSpec(memory_space=pltpu.VMEM)
    return pl.pallas_call(
        body,
        out_shape=jax.ShapeDtypeStruct((tok, width), BF),
        in_specs=[vm] * 6,
        out_specs=ANY,
        scratch_shapes=[
            pltpu.VMEM(part.shape, F32),
            pltpu.VMEM((tok, width), BF),
            pltpu.SemaphoreType.DMA((4,)),
        ],
        name="finish",
    )(*[in_vmem(a) for a in (ready, part, part_gain, power, one, two)])


U_CUTS = 4
D_CUTS = 2
LEAD = 3
FIRST = 3
ROUNDS = ((0,), (1,))


def routed():
    def grp_swap(v):
        return lax.ppermute(v, "grp", [(0, 1), (1, 0)])

    def y_swap(v):
        return lax.ppermute(v, "fs", [(i, i ^ 2) for i in range(4)])

    def core_swap(v):
        return lax.ppermute(v, "fs", [(i, i ^ 1) for i in range(4)])

    def tp_swap(v, m):
        return lax.ppermute(v, "tp", [(i, i ^ m) for i in range(4)])

    def per_device(prompt_tokens, up_weight, down_weight, pre_gain, post_gain):
        rows, hid = up_weight.shape
        tok, _ = prompt_tokens.shape
        half = rows // 2
        tile = hid // U_CUTS
        sub = half // D_CUTS

        def exchange(mine):
            got = y_swap(mine)
            near = core_swap(got)
            part = grp_swap(got)
            return [got, part, near, core_swap(part)]

        gain = pre_gain.reshape(1, rows)
        tops = [lambda i=i: (here()[2] * half, i * tile) for i in range(U_CUTS)]
        block = (half, tile)
        (lead,) = cast(up_weight, gain, [block], lambda: [tops[0]()])
        *second, r0 = cast(
            up_weight,
            gain,
            [block] * (LEAD - 1),
            lambda: [f() for f in tops[1:LEAD]],
            prompt_tokens,
        )
        up_own, *rest = cast(
            up_weight,
            gain,
            [(rows, hid)] + [block] * (U_CUTS - LEAD),
            lambda: [(0, 0)] + [f() for f in tops[LEAD:]],
        )
        down_own, *mine = cast(
            down_weight,
            None,
            [(rows, hid)] + [(sub, hid)] * D_CUTS,
            lambda: [(0, 0)] + [((2 * i + here()[2]) * sub, 0) for i in range(D_CUTS)],
        )
        up_far = [exchange(v) for v in [lead, *second, *rest]]
        down_far = [exchange(v) for v in mine]
        up_near = [up_own, core_swap(up_own)]
        down_near = [down_own, core_swap(down_own)]

        r2 = tp_swap(r0, 2)
        r1 = tp_swap(r0, 1)
        r3 = tp_swap(r2, 1)

        tiles = list(enumerate(up_far))
        cut = [(0, tok), (tok, tok), (2 * tok, tok)]
        hidden = list(feed([r1, r0, r2], up_near, tiles[:FIRST], [], None, []))
        *last, send1, keep0, keep2 = feed(
            [r1, r0, r2], up_near, tiles[FIRST:], hidden, down_near, cut
        )
        hidden = hidden + last
        got1 = tp_swap(send1, 1)
        *hidden3, send3 = feed([r3], up_near, tiles, [], down_near, cut[:1])
        near_terms = [keep0, got1, tp_swap(keep2, 2), tp_swap(send3, 3)]

        far_terms, sent = [], None
        cuts = [[(3 * tok, tok)], [cut[1]], [cut[2]], [cut[0]]]
        for ids in ROUNDS:
            send3, keep0, keep2, sent = down_far_step(
                [hidden, hidden3], [down_far[g] for g in ids], cuts, sub, sent
            )
            got3 = tp_swap(send3, 1)
            pair = add_rows(keep2, got3)
            far_terms.append([keep0, tp_swap(pair, 2)])
        one = tp_swap(sent, 1)
        two = far_terms[-1].pop()
        counts = [t[0].shape[1] for t in far_terms]
        state = before_last(near_terms, far_terms, post_gain, rows)

        def own_spots():
            y, core, _ = here()
            return [(pl.multiple_of((2 * y + c) * rows, 64), 0) for c in (core, 1 - core)]

        def up_spots():
            return [(a, i * tile) for i in range(U_CUTS) for a in up_places(rows, half)[2:]]

        def down_spots():
            y, core, grp = here()
            return [
                (pl.multiple_of((2 * (1 - y) + c) * rows + (2 * i + side) * sub, 64), 0)
                for i in range(D_CUTS)
                for c in (core, 1 - core)
                for side in (grp, 1 - grp)
            ]

        shape = (4 * rows, hid)
        whole_up = assemble(up_near, shape, own_spots)
        whole_up = assemble([p for g in up_far for p in g], shape, up_spots, whole_up)
        whole_down = assemble(down_near, shape, own_spots)
        whole_down = assemble([p for g in down_far for p in g], shape, down_spots, whole_down)
        mixed = finish(*state, one, two, counts, rows)
        return mixed, whole_up, whole_down

    return per_device


def solution(mesh):
    placed = (P(("grp", "fs", "tp"), None), P("fs", "tp"), P("fs", "tp"), P("fs"), P())
    fits = all(mesh.shape[a] == n for a, n in (("grp", 2), ("fs", 4), ("tp", 4)))
    return jax.shard_map(
        routed() if fits else plain,
        mesh=mesh,
        in_specs=placed,
        out_specs=(P(("grp", "fs", "tp"), None), P("grp", "tp"), P("grp", "tp")),
        check_vma=False,
    )
```

```python
import jax
import jax.numpy as jnp
from jax import lax
from jax.experimental import pallas as pl
from jax.experimental.pallas import tpu as pltpu
from jax.sharding import PartitionSpec as P


BF = jnp.bfloat16
F32 = jnp.float32
ANY = pl.BlockSpec(memory_space=pl.ANY)
LIMIT = pltpu.CompilerParams(vmem_limit_bytes=28 * 2**20)


def plain(prompt_tokens, up_weight, down_weight, pre_gain, post_gain):
    up_local = (up_weight * pre_gain[:, None]).astype(BF)
    down_local = down_weight.astype(BF)
    values = prompt_tokens.astype(F32)
    normed = (
        values * lax.rsqrt(jnp.mean(values * values, axis=1, keepdims=True) + 1e-06)
    ).astype(BF)
    sampler_up = lax.all_gather(up_local, "fs", axis=0, tiled=True)
    sampler_down = lax.all_gather(down_local, "fs", axis=0, tiled=True)
    lifted = jnp.dot(
        lax.all_gather(normed, "tp", axis=0, tiled=True),
        sampler_up,
        preferred_element_type=F32,
    )
    hidden = jnp.square(jax.nn.relu(lifted)).astype(BF)
    part = lax.dot_general(
        hidden, sampler_down, (((1,), (1,)), ((), ())), preferred_element_type=F32
    )
    summed = lax.psum_scatter(
        part.astype(BF), "tp", scatter_dimension=0, tiled=True
    ).astype(F32)
    scaled = summed * lax.rsqrt(jnp.mean(summed * summed, axis=1, keepdims=True) + 1e-06)
    return (scaled * post_gain[None, :]).astype(BF), sampler_up, sampler_down


def in_hbm(x):
    return pltpu.with_memory_space_constraint(x, pltpu.HBM)


def in_vmem(x):
    return pltpu.with_memory_space_constraint(x, pltpu.VMEM)


def hbm_call(body, out_shape, args, **options):
    many = isinstance(out_shape, (tuple, list))
    return pl.pallas_call(
        body,
        out_shape=out_shape,
        in_specs=[ANY] * len(args),
        out_specs=tuple([ANY] * len(out_shape)) if many else ANY,
        **options,
    )(*args)


class Copies:
    def __init__(self, sems):
        self.sems, self.used = sems, 0

    def start(self, src, dst):
        c = pltpu.make_async_copy(src, dst, self.sems.at[self.used])
        self.used += 1
        c.start()
        return c


def wait_all(copies):
    for c in copies:
        c.wait()


def here():
    fs = lax.axis_index("fs")
    return fs // 2, fs % 2, lax.axis_index("grp")


def up_places(rows, half):
    y, core, grp = here()
    near = [(2 * y + core) * rows, (2 * y + 1 - core) * rows]
    far = [
        (2 * (1 - y) + c) * rows + side * half
        for c in (core, 1 - core)
        for side in (grp, 1 - grp)
    ]
    return [pl.multiple_of(a, 128) for a in near + far]


def cast(weight, gain, wanted, places, tokens=None, step=64):
    rows, hid = weight.shape
    n = len(wanted)
    whole = [w == (rows, hid) for w in wanted]
    parts = [(i, r) for i, w in enumerate(wanted) for r in range(0, w[0], step)]
    full = any(whole)
    if tokens is not None:
        tok, width = tokens.shape
        token_rows = [(r, tok // 2) for r in range(0, tok, tok // 2)]

    def body(*refs):
        w, refs = refs[0], refs[1:]
        if gain is not None:
            g, refs = refs[0], refs[1:]
        if tokens is not None:
            t, refs = refs[0], refs[1:]
        outs, refs = refs[:n], refs[n:]
        if tokens is not None:
            normed, refs = refs[0], refs[1:]
        src, bufs, refs = refs[0], refs[1 : 1 + n], refs[1 + n :]
        if gain is not None:
            line_in, column, refs = refs[0], refs[1], refs[2:]
        if tokens is not None:
            token_in, token_out, refs = refs[0], refs[1], refs[2:]
        go = Copies(refs[0])
        at = places()
        stores = []
        if gain is not None:
            line = go.start(g, line_in)

        if tokens is not None:
            token_loads = [
                go.start(t.at[r : r + c, :], token_in.at[r : r + c, :]) for r, c in token_rows
            ]

        def scaled(v, row, count):
            if gain is None:
                return v.astype(BF)
            return (v * column[pl.ds(row, count), :]).astype(BF)

        if full:
            loads = [
                go.start(w.at[r : r + step, :], src.at[r : r + step, :])
                for r in range(0, rows, step)
            ]
        else:
            loads = []
            for i, r in parts:
                row, col = at[i]
                loads.append(
                    go.start(
                        w.at[pl.ds(pl.multiple_of(row + r, 8), step), pl.ds(col, wanted[i][1])],
                        src.at[r : r + step, pl.ds(col, wanted[i][1])],
                    )
                )
        if gain is not None:
            line.wait()
            column[...] = jnp.broadcast_to(line_in[...], (128, rows)).T[:, :1]
        if tokens is not None:
            for load, (r, count) in zip(token_loads, token_rows):
                load.wait()
                v = token_in[r : r + count, :].astype(F32)
                token_out[r : r + count, :] = (
                    v * lax.rsqrt(jnp.mean(v * v, axis=1, keepdims=True) + 1e-06)
                ).astype(BF)
                stores.append(
                    go.start(token_out.at[r : r + count, :], normed.at[r : r + count, :])
                )
        if full:
            for k, r in enumerate(range(0, rows, step)):
                loads[k].wait()
                i = whole.index(True)
                bufs[i][r : r + step, :] = scaled(src[r : r + step, :], r, step)
                stores.append(go.start(bufs[i].at[r : r + step, :], outs[i].at[r : r + step, :]))
            for j in range(n):
                if not whole[j]:
                    row, col = at[j]
                    stores.append(
                        go.start(
                            bufs[i].at[
                                pl.ds(pl.multiple_of(row, 16), wanted[j][0]),
                                pl.ds(col, wanted[j][1]),
                            ],
                            outs[j],
                        )
                    )
        else:
            for k, (i, r) in enumerate(parts):
                row, col = at[i]
                loads[k].wait()
                bufs[i][r : r + step, :] = scaled(
                    src[r : r + step, col : col + wanted[i][1]], row + r, step
                )
                stores.append(go.start(bufs[i].at[r : r + step, :], outs[i].at[r : r + step, :]))
        wait_all(stores)

    out_shape = [jax.ShapeDtypeStruct(w, BF) for w in wanted]
    scratch = [pltpu.VMEM((rows, hid) if n else (8, 128), F32)]
    scratch += [pltpu.VMEM(w, BF) for w in wanted]
    args = [in_hbm(weight)]
    if gain is not None:
        args.append(in_hbm(gain))
        scratch += [pltpu.VMEM((1, rows), F32), pltpu.VMEM((rows, 1), F32)]
    if tokens is not None:
        args.append(in_hbm(tokens))
        out_shape.append(jax.ShapeDtypeStruct((tok, width), BF))
        scratch += [pltpu.VMEM((tok, width), BF), pltpu.VMEM((tok, width), BF)]
    n_sem = 2 * rows // step + n + 2 * len(parts) + 8
    return hbm_call(
        body,
        tuple(out_shape),
        args,
        scratch_shapes=scratch + [pltpu.SemaphoreType.DMA((n_sem,))],
        compiler_params=LIMIT,
        cost_estimate=pl.CostEstimate(
            flops=10**8, bytes_accessed=6 * rows * hid, transcendentals=0
        ),
        name="cast",
    )


def feed(blocks, near, chunks, prev, down_near, cuts, whole=False, n_chunk=512):
    tok, width = blocks[0].shape
    rows, hid = near[0].shape
    half = rows // 2
    tile = chunks[0][1][0].shape[1]
    nb, nc, npv = len(blocks), len(chunks), len(prev)
    n_tok = nb * tok
    nf = len(chunks[0][1])
    n_in = nb + 2 + nc * nf + npv + (2 if down_near else 0)
    n_out = nc + (len(cuts) if down_near else 0) + 2 * whole
    n_sem = n_in + nc * 3 + n_out * (2 * rows // n_chunk + 1)

    def body(*refs):
        ins, outs, scratch = refs[:n_in], refs[n_in : n_in + n_out], refs[n_in + n_out :]
        x, w, h, sems = scratch[0], scratch[1], scratch[2], scratch[-1]
        go = Copies(sems)
        tok_in, ins = ins[:nb], ins[nb:]
        near_in, ins = ins[:2], ins[2:]
        loads = [go.start(tok_in[b], x.at[b * tok : (b + 1) * tok, :]) for b in range(nb)]
        at = up_places(rows, half)
        per_tile = []
        for k, (t, _) in enumerate(chunks):
            far, ins = ins[:nf], ins[nf:]
            cols = pl.ds(t * tile, tile)
            srcs = [a.at[:, cols] for a in near_in] + list(far)
            sizes = [rows, rows] + [half] * nf
            per_tile.append(
                [
                    go.start(src, w.at[k, pl.ds(a, size), :])
                    for src, a, size in zip(srcs, at, sizes)
                ]
            )
        late = [go.start(ins[i], h.at[:, i * tile : (i + 1) * tile]) for i in range(npv)]
        ins = ins[npv:]
        if down_near:
            d, o = scratch[3], scratch[4]
            core = here()[1]
            late.append(go.start(ins[0], d.at[pl.ds(pl.multiple_of(core * rows, 128), rows), :]))
            late.append(
                go.start(ins[1], d.at[pl.ds(pl.multiple_of((1 - core) * rows, 128), rows), :])
            )
        wait_all(loads)
        stores = []
        for k, (t, _) in enumerate(chunks):
            wait_all(per_tile[k])
            if whole:
                stores.append(go.start(w.at[k], outs[-2].at[:, pl.ds(t * tile, tile)]))
            for c in range(0, tile, n_chunk):
                n = min(n_chunk, tile)
                lifted = jnp.dot(x[...], w[k, :, c : c + n], preferred_element_type=F32)
                h[:, t * tile + c : t * tile + c + n] = jnp.square(
                    jnp.maximum(lifted, 0.0)
                ).astype(BF)
            stores.append(go.start(h.at[:, t * tile : (t + 1) * tile], outs[k]))
        wait_all(late)
        if whole:
            first = pl.multiple_of(here()[0] * 2 * rows, 128)
            stores.append(go.start(d, outs[-1].at[pl.ds(first, 2 * rows), :]))
        if down_near:
            for c in range(0, 2 * rows, n_chunk):
                o[:, c : c + n_chunk] = lax.dot_general(
                    h[...],
                    d[c : c + n_chunk, :],
                    (((1,), (1,)), ((), ())),
                    preferred_element_type=F32,
                ).astype(BF)
                for out, (first, count) in zip(outs[nc:], cuts):
                    stores.append(
                        go.start(
                            o.at[first : first + count, c : c + n_chunk],
                            out.at[:, c : c + n_chunk],
                        )
                    )
        wait_all(stores)

    out_shape = [jax.ShapeDtypeStruct((n_tok, tile), BF)] * nc
    scratch = [
        pltpu.VMEM((n_tok, width), BF),
        pltpu.VMEM((nc, width, tile), BF),
        pltpu.VMEM((n_tok, hid), BF),
    ]
    flops = 2 * n_tok * width * tile * nc
    if down_near:
        out_shape += [
            pltpu.HBM((count, 2 * rows), BF)
            if i == 1
            else jax.ShapeDtypeStruct((count, 2 * rows), BF)
            for i, (_, count) in enumerate(cuts)
        ]
        scratch += [pltpu.VMEM((2 * rows, hid), BF), pltpu.VMEM((n_tok, 2 * rows), BF)]
        flops += 2 * n_tok * hid * 2 * rows
    if whole:
        out_shape += [jax.ShapeDtypeStruct((4 * rows, hid), BF)] * 2
    args = list(blocks) + list(near)
    for _, far in chunks:
        args += far
    args += list(prev) + list(down_near or [])
    return hbm_call(
        body,
        tuple(out_shape),
        args,
        scratch_shapes=scratch + [pltpu.SemaphoreType.DMA((n_sem,))],
        compiler_params=LIMIT,
        cost_estimate=pl.CostEstimate(
            flops=flops, bytes_accessed=2 * width * tile * nc, transcendentals=0
        ),
        name="feed",
    )


def down_far_step(hiddens, groups, cuts, sub, before, whole, first_group):
    hid = groups[0][0].shape[1]
    n_groups, nf = len(groups), len(groups[0])
    counts = [h[0].shape[0] for h in hiddens]
    n_tok = sum(counts)
    n_h = sum(len(h) for h in hiddens)
    cols = n_groups * nf * sub
    ahead = 0 if before is None else before.shape[1]
    n_in = n_h + n_groups * nf + (ahead > 0) + 1
    n_out = len(cuts) + 1
    rows = whole.shape[0] // 4

    def body(*refs):
        ins, outs = refs[:n_in], refs[n_in : n_in + len(cuts)]
        whole_out, h, d, o, sems = refs[n_in + len(cuts) :]
        go = Copies(sems)
        loads, k, r0 = [], 0, 0
        for tiles, count in zip(hiddens, counts):
            c0 = 0
            for t in tiles:
                loads.append(go.start(ins[k], h.at[r0 : r0 + count, c0 : c0 + t.shape[1]]))
                c0 += t.shape[1]
                k += 1
            r0 += count
        _, core, grp = here()
        for g in range(n_groups):
            place = [
                c * (cols // 2) + g * 2 * sub + side * sub
                for c in (core, 1 - core)
                for side in (grp, 1 - grp)
            ]
            for a in place:
                loads.append(go.start(ins[k], d.at[pl.ds(pl.multiple_of(a, 64), sub), :]))
                k += 1
        stores = []
        if ahead:
            stores.append(go.start(ins[k], outs[-1].at[:, :ahead]))
        wait_all(loads)
        for c in range(2):
            to = (2 * (1 - here()[0]) + c) * rows + first_group * 2 * sub
            stores.append(
                go.start(
                    d.at[c * (cols // 2) : (c + 1) * (cols // 2), :],
                    whole_out.at[pl.ds(pl.multiple_of(to, 128), cols // 2), :],
                )
            )
        o[...] = lax.dot_general(
            h[...], d[...], (((1,), (1,)), ((), ())), preferred_element_type=F32
        ).astype(BF)
        for q, (out, runs) in enumerate(zip(outs, cuts)):
            r0 = 0
            for first, count in runs:
                to = pl.ds(ahead if q == len(cuts) - 1 else 0, cols)
                stores.append(
                    go.start(o.at[first : first + count, :], out.at[r0 : r0 + count, to])
                )
                r0 += count
        wait_all(stores)

    return hbm_call(
        body,
        tuple(
            (pltpu.HBM if i == 1 else jax.ShapeDtypeStruct)(
                (sum(c for _, c in runs), cols + (ahead if i == len(cuts) - 1 else 0)), BF
            )
            for i, runs in enumerate(cuts)
        )
        + (jax.ShapeDtypeStruct(whole.shape, BF),),
        [t for h in hiddens for t in h]
        + [p for g in groups for p in g]
        + ([before] if ahead else [])
        + [whole],
        input_output_aliases={n_in - 1: n_out - 1},
        scratch_shapes=[
            pltpu.VMEM((n_tok, hid), BF),
            pltpu.VMEM((cols, hid), BF),
            pltpu.VMEM((n_tok, cols), BF),
            pltpu.SemaphoreType.DMA((n_in + 2 + sum(len(r) for r in cuts),)),
        ],
        compiler_params=LIMIT,
        cost_estimate=pl.CostEstimate(
            flops=2 * n_tok * cols * hid, bytes_accessed=2 * cols * hid, transcendentals=0
        ),
        name="down_far",
    )


def add_rows(keep, got):
    return (keep.astype(F32) + got.astype(F32)).astype(BF)


def before_last(near, far, post_gain, rows):
    width = 4 * rows
    terms = [near] + far
    flat = [a for t in terms for a in t]
    tok = near[0].shape[0]
    counts = [t[0].shape[1] for t in terms]
    n_far = sum(counts[1:])

    def body(*refs):
        n_in = 1 + len(flat)
        o, part, part_gain, power = refs[n_in : n_in + 4]
        local, sems = refs[n_in + 4 : -1], refs[-1]
        go = Copies(sems)
        wait_all([go.start(a.at[: b.shape[0]], b) for a, b in zip(refs[:n_in], local)])
        gain, ins = local[0], list(local[1:])
        sums = []
        for t in terms:
            group, ins = ins[: len(t)], ins[len(t) :]
            sums.append(sum(g[...].astype(F32) for g in group))
        total = jnp.sum(sums[0] * sums[0], axis=1, keepdims=True)
        power[...] = jnp.broadcast_to(total, (tok, 128))
        at = 0
        for s in sums[1:]:
            part[:, at : at + s.shape[1]] = s
            at += s.shape[1]
        for y in range(2):

            @pl.when(here()[0] == y)
            def _(y=y):
                place = near_place(y, rows)
                o[:, place] = sums[0] * gain[:, place]
                for place, at, n in far_places(y, rows, counts[1:]):
                    part_gain[:, at : at + n] = gain[:, place]

    vm = pl.BlockSpec(memory_space=pltpu.VMEM)
    return pl.pallas_call(
        body,
        out_shape=(
            pltpu.VMEM((tok, width), F32),
            pltpu.VMEM((tok, n_far), F32),
            pltpu.VMEM((1, n_far), F32),
            pltpu.VMEM((tok, 128), F32),
        ),
        in_specs=[ANY] * (1 + len(flat)),
        out_specs=(vm,) * 4,
        scratch_shapes=[pltpu.VMEM((1, width), F32)]
        + [pltpu.VMEM((tok, a.shape[1]), BF) for a in flat]
        + [pltpu.SemaphoreType.DMA((1 + len(flat),))],
        name="before_last",
    )(post_gain.reshape(1, width), *flat)


def near_place(y, rows):
    return slice(y * 2 * rows, (y + 1) * 2 * rows)


def far_places(y, rows, counts):
    found, at, before = [], 0, 0
    for count in counts:
        n = count // 2
        for c in range(2):
            start = (1 - y) * 2 * rows + c * rows + before
            found.append((slice(start, start + n), at, n))
            at += n
        before += n
    return found


def finish(ready, part, part_gain, power, one, two, counts, rows):
    tok, width = ready.shape
    n_two = two.shape[1]

    def body(r, p, g, w, a, b, out, v, o, sems):
        v[...] = p[...] + a[...].astype(F32)
        v[:, -n_two:] += b[...].astype(F32)
        total = w[:, :1] + jnp.sum(v[...] * v[...], axis=1, keepdims=True)
        scale = lax.rsqrt(total / width + 1e-06)
        go = Copies(sems)
        step = tok // 4
        stores = []
        for r0 in range(0, tok, step):
            own = slice(r0, r0 + step)
            for y in range(2):

                @pl.when(here()[0] == y)
                def _(y=y):
                    place = near_place(y, rows)
                    o[own, place] = (r[own, place] * scale[own]).astype(BF)
                    for place, at, n in far_places(y, rows, counts):
                        cols = slice(at, at + n)
                        o[own, place] = (v[own, cols] * g[:, cols] * scale[own]).astype(BF)

            stores.append(go.start(o.at[own, :], out.at[own, :]))
        wait_all(stores)

    vm = pl.BlockSpec(memory_space=pltpu.VMEM)
    return pl.pallas_call(
        body,
        out_shape=jax.ShapeDtypeStruct((tok, width), BF),
        in_specs=[vm] * 6,
        out_specs=ANY,
        scratch_shapes=[
            pltpu.VMEM(part.shape, F32),
            pltpu.VMEM((tok, width), BF),
            pltpu.SemaphoreType.DMA((4,)),
        ],
        name="finish",
    )(*[in_vmem(a) for a in (ready, part, part_gain, power, one, two)])


U_CUTS = 4
D_CUTS = 4
LEAD = 3
FIRST = 3
ROUNDS = ((0, 1), (2, 3))


def routed():
    def grp_swap(v):
        return lax.ppermute(v, "grp", [(0, 1), (1, 0)])

    def y_swap(v):
        return lax.ppermute(v, "fs", [(i, i ^ 2) for i in range(4)])

    def core_swap(v):
        return lax.ppermute(v, "fs", [(i, i ^ 1) for i in range(4)])

    def tp_swap(v, m):
        return lax.ppermute(v, "tp", [(i, i ^ m) for i in range(4)])

    def per_device(prompt_tokens, up_weight, down_weight, pre_gain, post_gain):
        rows, hid = up_weight.shape
        tok, _ = prompt_tokens.shape
        half = rows // 2
        tile = hid // U_CUTS
        sub = half // D_CUTS

        def exchange(mine):
            got = y_swap(mine)
            near = core_swap(got)
            part = grp_swap(got)
            return [got, part, near, core_swap(part)]

        gain = pre_gain.reshape(1, rows)
        tops = [lambda i=i: (here()[2] * half, i * tile) for i in range(U_CUTS)]
        block = (half, tile)
        (lead,) = cast(up_weight, gain, [block], lambda: [tops[0]()])
        *second, r0 = cast(
            up_weight,
            gain,
            [block] * (LEAD - 1),
            lambda: [f() for f in tops[1:LEAD]],
            prompt_tokens,
        )
        up_own, *rest = cast(
            up_weight,
            gain,
            [(rows, hid)] + [block] * (U_CUTS - LEAD),
            lambda: [(0, 0)] + [f() for f in tops[LEAD:]],
        )
        down_own, *mine = cast(
            down_weight,
            None,
            [(rows, hid)] + [(sub, hid)] * D_CUTS,
            lambda: [(0, 0)] + [((2 * i + here()[2]) * sub, 0) for i in range(D_CUTS)],
        )
        up_far = [exchange(v) for v in [lead, *second, *rest]]
        down_far = [exchange(v) for v in mine]
        up_near = [up_own, core_swap(up_own)]
        down_near = [down_own, core_swap(down_own)]

        r2 = tp_swap(r0, 2)
        r1 = tp_swap(r0, 1)
        r3 = tp_swap(r2, 1)

        tiles = list(enumerate(up_far))
        cut = [(0, tok), (tok, tok), (2 * tok, tok)]
        hidden = list(feed([r1, r0, r2], up_near, tiles[:FIRST], [], None, []))
        *last, send1, keep0, keep2 = feed(
            [r1, r0, r2], up_near, tiles[FIRST:], hidden, down_near, cut
        )
        hidden = hidden + last
        got1 = tp_swap(send1, 1)
        *hidden3, send3, whole_up, whole_down = feed(
            [r3], up_near, tiles, [], down_near, cut[:1], True
        )
        near_terms = [keep0, got1, tp_swap(keep2, 2), tp_swap(send3, 3)]

        far_terms, sent = [], None
        cuts = [[(3 * tok, tok)], [cut[1]], [cut[2]], [cut[0]]]
        for ids in ROUNDS:
            send3, keep0, keep2, sent, whole_down = down_far_step(
                [hidden, hidden3], [down_far[g] for g in ids], cuts, sub, sent, whole_down, ids[0]
            )
            got3 = tp_swap(send3, 1)
            pair = add_rows(keep2, got3)
            far_terms.append([keep0, tp_swap(pair, 2)])
        one = tp_swap(sent, 1)
        two = far_terms[-1].pop()
        counts = [t[0].shape[1] for t in far_terms]
        state = before_last(near_terms, far_terms, post_gain, rows)

        mixed = finish(*state, one, two, counts, rows)
        return mixed, whole_up, whole_down

    return per_device


def solution(mesh):
    placed = (P(("grp", "fs", "tp"), None), P("fs", "tp"), P("fs", "tp"), P("fs"), P())
    fits = all(mesh.shape[a] == n for a, n in (("grp", 2), ("fs", 4), ("tp", 4)))
    return jax.shard_map(
        routed() if fits else plain,
        mesh=mesh,
        in_specs=placed,
        out_specs=(P(("grp", "fs", "tp"), None), P("grp", "tp"), P("grp", "tp")),
        check_vma=False,
    )
```
